32 devices in a mesh: ep: 8 (over z, x), tp: 4 (over y, core).
Axes of the slice: x: 2, y: 2, z: 4, core: 2. Of those that a mesh axis runs over, the one named last changes fastest.
Arguments:
- queries: bfloat16 [4096, 2048], P('ep', 'tp'), may hold values from -6 to 6
- keys: bfloat16 [4096, 2048], P('ep', 'tp'), may hold values from -12 to 12
- values: bfloat16 [4096, 2048], P('ep', 'tp'), may hold values from -8 to 8
- key_bias: bfloat16 [4096, 16], P('ep', 'tp'), may hold values from -16 to 0
- out_weight: bfloat16 [2048, 2048], P('tp'), may hold values from -0.1875 to 0.1875
- moe_input: bfloat16 [1024, 2048], P('ep'), may hold values from -6 to 6
- moe_gain: float32 [2048], replicated, may hold values from 0.1 to 1.9
- route_ids: int32 [1024, 2], P('ep'), may hold values from 0 to 7, all different within a row; in each aligned block of 128 rows (0 to 127, 128 to 255, ...) at most 48 rows name the same one
- route_scores: float32 [1024, 2], P('ep'), may hold values from 0.05 to 1
- shared_gate: bfloat16 [2048, 2048], P(None, 'tp'), may hold values from -0.125 to 0.125
- shared_up: bfloat16 [2048, 2048], P(None, 'tp'), may hold values from -0.125 to 0.125
- shared_down: bfloat16 [2048, 2048], P('tp'), may hold values from -0.1875 to 0.1875
- expert_gate: bfloat16 [8, 2048, 2048], P('ep', None, 'tp'), may hold values from -0.125 to 0.125
- expert_up: bfloat16 [8, 2048, 2048], P('ep', None, 'tp'), may hold values from -0.125 to 0.125
- expert_down: bfloat16 [8, 2048, 2048], P('ep', 'tp'), may hold values from -0.1875 to 0.1875
Outputs:
- mixed_tokens: bfloat16 [4096, 2048], P('ep', 'tp')
- expert_mix: bfloat16 [1024, 2048], P('ep', 'tp')
The draws below stay inside these ranges and needn't reach their ends.
Inputs may be any that keep to these rules, and one draw needn't show every extreme that they name: `route_ids`: each row names 2 different experts. Among the 128 rows of one index of ep no expert is named by more than 48 rows, and in some such block one expert is named by exactly 48 rows.
All inputs are finite; a program needn't handle non-finite values.
Results may differ from the reference program's by a relative error of at most 0.019.
Values may be sent and summed in bfloat16 or wider, within the bound.
A program may use at most 128 MiB of HBM per device.

```python
import math
import jax
import jax.numpy as jnp
import numpy as np
from jax import lax

D = 2048
HEADS = 16
HD = 128
F = 2048
FSH = 2048
TOPK = 2
SEQUENCE_COUNT = 1
ROWS_A = 512
ROWS_M = 128
ATTENTION_TOKENS = 4096
SEQUENCE_LENGTH = 4096
TOKENS_M = 1024
EXPERTS = 8
CAP = 48
N_EP = 8
N_TP = 4


def draw_key_bias(key, part):
    draw_keys = jax.random.split(key, 7)
    fast_share = 0.5
    fast_head = jax.random.uniform(draw_keys[0], (HEADS,)) < fast_share
    fast_rate = jnp.exp(jax.random.uniform(draw_keys[1], (HEADS,), minval=jnp.log(1.0 / 100.0), maxval=jnp.log(1.0 / 30.0)))
    slow_rate = jnp.exp(jax.random.uniform(draw_keys[2], (HEADS,), minval=jnp.log(0.3 / SEQUENCE_LENGTH), maxval=jnp.log(1.2 / SEQUENCE_LENGTH)))
    base_logit = jnp.log(jnp.where(fast_head, fast_rate, slow_rate)) - 2.15
    block_count = ATTENTION_TOKENS // ROWS_A
    block_shift = jax.random.uniform(draw_keys[3], (block_count, 1, HEADS), minval=-0.7, maxval=0.7)
    jitter = jax.random.uniform(draw_keys[4], (block_count, ROWS_A, HEADS), minval=-0.7, maxval=0.7)
    smoothing_factor = (base_logit[None, None, :] + block_shift + jitter).reshape(ATTENTION_TOKENS, HEADS)
    spike_position = jax.random.randint(draw_keys[5], (SEQUENCE_COUNT, 2), 0, SEQUENCE_LENGTH)
    token_position = jnp.arange(ATTENTION_TOKENS) % SEQUENCE_LENGTH
    sequence_index = jnp.arange(ATTENTION_TOKENS) // SEQUENCE_LENGTH
    spike_mask = jnp.any(token_position[:, None] == spike_position[sequence_index], axis=1)
    spike_fraction = jax.random.uniform(draw_keys[6], (ATTENTION_TOKENS, 1), minval=0.2, maxval=0.4)
    spike_logit = jnp.log(spike_fraction) - jnp.log(1.0 - spike_fraction)
    return jnp.where(spike_mask[:, None], spike_logit, smoothing_factor).astype(jnp.float32).astype(jnp.bfloat16)


def draw_values(key, part):
    draw_keys = jax.random.split(key, 3)
    block_count = ATTENTION_TOKENS // ROWS_A
    sign = jnp.where(jax.random.uniform(draw_keys[0], (HEADS,)) < 0.5, -1.0, 1.0)
    size = jax.random.uniform(draw_keys[1], (block_count, 1, HEADS, 1), minval=0.5, maxval=1.5)
    noise = jnp.clip(1.5 * jax.random.normal(draw_keys[2], (block_count, ROWS_A, HEADS, HD)), -6.0, 6.0)
    mixed = sign[None, None, :, None] * size + noise
    return mixed.reshape(ATTENTION_TOKENS, HEADS * HD).astype(jnp.float32).astype(jnp.bfloat16)


def with_spikes(array, rng, source, target, blocks, factor):
    def block_of(axis_at):
        return (jnp.arange(array.shape[axis_at]) // (array.shape[axis_at] // blocks)).reshape((-1,) + (1,) * (array.ndim - 1 - axis_at))

    one_side = jax.random.permutation(rng, blocks)[block_of(target)]
    far = (block_of(target) + blocks // 2) % blocks
    return jnp.where((block_of(source) == one_side) | (block_of(source) == far), factor * array, array)


def level_of(rng, extent, cuts, low, top_value):
    gain = 1.0
    for position, shards_of in cuts:
        heights = jax.random.uniform(jax.random.fold_in(jax.random.fold_in(rng, 6), position), (shards_of,), jnp.float32, low / len(cuts), top_value / len(cuts))
        gain = gain * jnp.repeat(jnp.exp(heights), extent[position] // shards_of).reshape((-1,) + (1,) * (len(extent) - 1 - position))
    return gain


def routed_block(key, own, number, rows, count, top, most, slope):
    order = jax.random.permutation(key, count)
    crowded, usual = portions_of(count, rows * top, most, slope, True), portions_of(count, rows * top, most, slope, False)
    places = jnp.arange(count)

    def named(lengths, offset_by):
        used = int((lengths > 0).sum())
        fixed = max(1, used // 4)
        shifted = fixed + (places - fixed + offset_by * (used - fixed)) % max(1, count - fixed)
        return jnp.zeros((count,), jnp.int32).at[order[jnp.where(places < fixed, places, shifted)]].set(jnp.asarray(lengths, jnp.int32))

    lengths = jnp.where(number % 4 == 0, named(crowded, number // 4), named(usual, number - number // 4 - 1))
    mixed = jax.random.permutation(jax.random.fold_in(own, 3), count)
    donor, sink = mixed[0:count // 2 * 2:2], mixed[1:count // 2 * 2:2]
    slack = jnp.minimum(lengths[donor] - 1, most - lengths[sink]) // 2
    slack = jnp.where((donor == order[0]) | (sink == order[0]) | (lengths[sink] == 0), 0, jnp.maximum(slack, 0))
    shifted = jax.random.randint(jax.random.fold_in(own, 4), (count // 2,), 0, 1 << 20) % (slack + 1)
    lengths = lengths.at[donor].add(-shifted).at[sink].add(shifted)
    members = jnp.searchsorted(jnp.cumsum(lengths), jnp.arange(rows * top), side="right").astype(jnp.int32)
    table = members.reshape(top, rows).T
    table = table[jax.random.permutation(jax.random.fold_in(own, 1), rows)]
    offset_by = jax.random.randint(jax.random.fold_in(own, 2), (rows, 1), 0, top)
    return jnp.take_along_axis(table, (jnp.arange(top)[None, :] + offset_by) % top, axis=1)


def portions_of(count, total, limit, lean, full):
    portions = [(1 << 20) // math.isqrt(standing ** lean) + 1 for standing in range(1, count + 1)]
    largest = limit if full else min(limit, max(-(-total // count), total * portions[0] // sum(portions)))
    least = 1 if total - largest >= count - 1 else 0
    holding, surplus = [largest] + [least] * (count - 1), total - largest - least * (count - 1)
    while surplus > 0:
        free = [i for i in range(1, count) if holding[i] < largest] or [i for i in range(1, count) if holding[i] < limit]
        mass, left = sum([portions[i] for i in free]), surplus
        for i in free:
            extra = min(limit - holding[i], max(1, left * portions[i] // mass), surplus)
            holding[i] = holding[i] + extra
            surplus = surplus - extra
    return np.array(holding)


def centred(rng, extent, deviation, most, shards=(), kind=jnp.bfloat16):
    gain = level_of(rng, extent, shards, -0.22, 0.18) if shards else 1.0
    values = jax.random.normal(rng, extent, jnp.float32) * deviation * gain
    return jnp.minimum(jnp.maximum(values, -most), most).astype(kind)


def gaussian_with(stream_key, dims, scale, limit, shards, heavy, held_as=jnp.bfloat16):
    array = scale * jax.random.normal(stream_key, dims, jnp.float32)
    if shards:
        array = array * level_of(stream_key, dims, shards, -0.22, 0.18)
    return jnp.clip(with_spikes(array, jax.random.fold_in(stream_key, 3), *heavy), -limit, limit).astype(held_as)


def setup_inputs(seed: int = 0) -> dict:
    streams_of = jax.random.split(jax.random.key(seed), 16)
    queries = centred(streams_of[0], (ATTENTION_TOKENS, HEADS * HD), 1.0, 6.0, ((0, 8), (1, 4)))
    keys = centred(streams_of[1], (ATTENTION_TOKENS, HEADS * HD), 2.0, 12.0, ((0, 8), (1, 4)))
    values = draw_values(jax.random.fold_in(streams_of[15], 71), 0)
    key_bias = draw_key_bias(jax.random.fold_in(streams_of[15], 71), 0)
    out_weight = gaussian_with(streams_of[4], (HEADS * HD, D), (HEADS * HD) ** -0.5, 0.1875, ((0, 4),), (0, 1, 4, 2.0))
    moe_input = centred(streams_of[5], (TOKENS_M, D), 1.0, 6.0, ((0, 8),))
    moe_gain = jnp.clip(1.0 + 0.18 * jax.random.normal(streams_of[6], (D,), jnp.float32), 0.1, 1.9)
    route_ids_keys = jax.random.split(jax.random.fold_in(streams_of[7], 1), TOKENS_M // ROWS_M)
    route_ids_turns = jax.random.permutation(jax.random.fold_in(streams_of[7], 3), TOKENS_M // ROWS_M)
    route_ids = jax.vmap(lambda own, number: routed_block(jax.random.fold_in(streams_of[7], 2), own, number, ROWS_M, EXPERTS, TOPK, CAP, 2))(route_ids_keys, route_ids_turns).reshape((TOKENS_M, TOPK))
    route_scores = jnp.clip(0.05 + 0.95 * jax.random.uniform(streams_of[8], (TOKENS_M, TOPK), jnp.float32) ** level_of(streams_of[8], (TOKENS_M, TOPK), ((0, 8),), -0.2, 0.2), 0.05, 1.0)
    shared_gate = centred(streams_of[9], (D, FSH), D ** -0.5, 0.125, ((1, 4),))
    shared_up = centred(streams_of[10], (D, FSH), D ** -0.5, 0.125, ((1, 4),))
    shared_down = gaussian_with(streams_of[11], (FSH, D), FSH ** -0.5, 0.1875, ((0, 4),), (0, 1, 4, 2.0))
    expert_gate = centred(streams_of[12], (EXPERTS, D, F), D ** -0.5, 0.125, ((0, 8), (2, 4)))
    expert_up = centred(streams_of[13], (EXPERTS, D, F), D ** -0.5, 0.125, ((0, 8), (2, 4)))
    expert_down = gaussian_with(streams_of[14], (EXPERTS, F, D), F ** -0.5, 0.1875, ((0, 8), (1, 4)), (1, 2, 4, 2.0))
    return {"queries": queries, "keys": keys, "values": values, "key_bias": key_bias, "out_weight": out_weight, "moe_input": moe_input, "moe_gain": moe_gain, "route_ids": route_ids, "route_scores": route_scores, "shared_gate": shared_gate, "shared_up": shared_up, "shared_down": shared_down, "expert_gate": expert_gate, "expert_up": expert_up, "expert_down": expert_down}


EPS_NORM = 1e-06
ROUTED_SCALE = 2.5

def head_span(query_head, key_head, value_head, bias_head):
    length = query_head.shape[0]
    block = min(512, length)
    scale = HD ** (-0.5)
    key_pos = jnp.arange(length, dtype=jnp.int32)
    bias_row = bias_head.astype(jnp.float32)[None, :]

    def one_block(start):
        query_block = lax.dynamic_slice_in_dim(query_head, start, block, 0)
        logit = jnp.dot(query_block, key_head.T, preferred_element_type=jnp.float32) * scale + bias_row
        query_pos = start + jnp.arange(block, dtype=jnp.int32)
        visible = key_pos[None, :] < query_pos[:, None]
        keep = jnp.where(visible, jax.nn.log_sigmoid(-logit), 0.0)
        stay = lax.cumsum(keep, axis=1, reverse=True) - keep
        weight = jnp.where(visible, jnp.exp(jax.nn.log_sigmoid(logit) + stay), 0.0).astype(jnp.bfloat16)
        return jnp.dot(weight, value_head, preferred_element_type=jnp.float32).astype(jnp.bfloat16)
    starts = jnp.arange(length // block, dtype=jnp.int32) * block
    return lax.map(one_block, starts).reshape(length, -1)

def per_head(operands):
    return head_span(operands[0], operands[1], operands[2], operands[3])

def grouped_sum(left, right, groups):
    width = left.shape[1] // groups
    total = jnp.zeros((left.shape[0], right.shape[1]), jnp.float32)
    for group in range(groups):
        partial_sum = jnp.dot(left[:, group * width:(group + 1) * width], right[group * width:(group + 1) * width], preferred_element_type=jnp.float32)
        rounded = lax.optimization_barrier(partial_sum.astype(jnp.bfloat16))
        total = total + rounded.astype(jnp.float32)
    return total

def one_expert(operands):
    rows_in, weight_gate, weight_up, weight_down = operands
    gate_part = jnp.dot(rows_in, weight_gate, preferred_element_type=jnp.float32)
    up_part = jnp.dot(rows_in, weight_up, preferred_element_type=jnp.float32)
    hidden = (jax.nn.silu(gate_part) * up_part).astype(jnp.bfloat16)
    return grouped_sum(hidden, weight_down, N_TP).astype(jnp.bfloat16)

def reference(queries, keys, values, key_bias, out_weight, moe_input, moe_gain, route_ids, route_scores, shared_gate, shared_up, shared_down, expert_gate, expert_up, expert_down):
    pieces = []
    for sequence_index in range(SEQUENCE_COUNT):
        first = sequence_index * SEQUENCE_LENGTH
        query_seq = queries[first:first + SEQUENCE_LENGTH].reshape(SEQUENCE_LENGTH, HEADS, HD).transpose(1, 0, 2)
        key_seq = keys[first:first + SEQUENCE_LENGTH].reshape(SEQUENCE_LENGTH, HEADS, HD).transpose(1, 0, 2)
        value_seq = values[first:first + SEQUENCE_LENGTH].reshape(SEQUENCE_LENGTH, HEADS, HD).transpose(1, 0, 2)
        bias_seq = key_bias[first:first + SEQUENCE_LENGTH].T
        head_outs = lax.map(per_head, (query_seq, key_seq, value_seq, bias_seq))
        pieces.append(head_outs.transpose(1, 0, 2).reshape(SEQUENCE_LENGTH, HEADS * HD))
    heads_out = jnp.concatenate(pieces, axis=0)
    mixed_tokens = grouped_sum(heads_out, out_weight, N_TP).astype(jnp.bfloat16)
    inputs = moe_input.astype(jnp.float32)
    normed = (inputs * lax.rsqrt(lax.optimization_barrier(jnp.mean(inputs * inputs, axis=-1, keepdims=True)) + EPS_NORM) * moe_gain.astype(jnp.float32)).astype(jnp.bfloat16)
    shared_hidden = (jax.nn.silu(jnp.dot(normed, shared_gate, preferred_element_type=jnp.float32)) * jnp.dot(normed, shared_up, preferred_element_type=jnp.float32)).astype(jnp.bfloat16)
    shared_result = grouped_sum(shared_hidden, shared_down, N_TP)
    chosen = route_ids.reshape(N_EP, ROWS_M * TOPK).astype(jnp.int32)
    onehot = (chosen[:, :, None] == jnp.arange(EXPERTS, dtype=jnp.int32)[None, None, :]).astype(jnp.int32)
    place = lax.optimization_barrier(jnp.sum((jnp.cumsum(onehot, axis=1) - onehot) * onehot, axis=2))
    block_ids = jnp.arange(N_EP, dtype=jnp.int32)[:, None]
    slot_index = (chosen * (N_EP * CAP) + block_ids * CAP + place).reshape(-1).astype(jnp.int32)
    token_index = jnp.arange(TOKENS_M * TOPK, dtype=jnp.int32) // TOPK
    expert_rows = jnp.zeros((EXPERTS * N_EP * CAP, D), jnp.bfloat16).at[slot_index].set(normed[token_index])
    expert_rows = expert_rows.reshape(EXPERTS, N_EP * CAP, D)
    results = lax.map(one_expert, (expert_rows, expert_gate, expert_up, expert_down))
    results = results.reshape(EXPERTS * N_EP * CAP, D)
    picked = results[slot_index].astype(jnp.float32).reshape(TOKENS_M, TOPK, D)
    scores = route_scores.astype(jnp.float32)
    gates = scores / lax.optimization_barrier(jnp.sum(scores, axis=-1, keepdims=True)) * ROUTED_SCALE
    expert_mix = (shared_result + lax.optimization_barrier(jnp.sum(gates[:, :, None] * picked, axis=1))).astype(jnp.bfloat16)
    return (mixed_tokens, expert_mix)
```

```python
import functools

import jax
import jax.numpy as jnp
from jax import lax
from jax.experimental import pallas as pl
from jax.experimental.pallas import tpu as pltpu
from jax.sharding import PartitionSpec as P

EPS_NORM = 1e-06
ROUTED_SCALE = 2.5
LOG2E = 1.4426950408889634
BIAS_ROWS = 16


def attention_kernel(share, span, place_ref, data_ref, tri_ref, out_ref):
    block = pl.program_id(0)
    offset = place_ref[0] * share
    width = tri_ref.shape[0]
    size = out_ref.shape[2]
    query = data_ref[block, pl.ds(0, share), :]
    scale = size ** (-0.5) * LOG2E

    def unit(key_block, carry, masked):
        total, passed = carry
        key = data_ref[key_block, pl.ds(share, span), :]
        value = data_ref[key_block, pl.ds(share + span, span), :]
        bias = data_ref[key_block, pl.ds(share + 2 * span, BIAS_ROWS), :].astype(jnp.float32)
        bias = bias * LOG2E
        for start in range(span - width, -1, -width):
            row = jnp.concatenate(
                [
                    bias[i : i + 1, :]
                    for i in range(start // size, (start + width) // size)
                ],
                axis=1,
            )
            logit = (
                lax.dot_general(
                    query,
                    key[start : start + width],
                    (((1,), (1,)), ((), ())),
                    preferred_element_type=jnp.float32,
                )
                * scale
                + row
            )
            drop = jnp.maximum(logit, jnp.log(1.0 + jnp.exp2(jnp.minimum(logit, 126.0))) * LOG2E)
            base = logit - drop
            if masked:
                shape = (share, width)
                visible = start + lax.broadcasted_iota(
                    jnp.int32, shape, 1
                ) < offset + lax.broadcasted_iota(jnp.int32, shape, 0)
                drop = jnp.where(visible, drop, 0.0)
            later = jnp.dot(
                drop.astype(jnp.bfloat16), tri_ref[...], preferred_element_type=jnp.float32
            )
            weight = jnp.exp2(base - later - passed)
            if masked:
                weight = jnp.where(visible, weight, 0.0)
            passed = passed + later[:, 0:1] + drop[:, 0:1]
            total = total + jnp.dot(
                weight.astype(jnp.bfloat16),
                value[start : start + width],
                preferred_element_type=jnp.float32,
            )
        return (total, passed)

    carry = (jnp.zeros((share, size), jnp.float32), jnp.zeros((share, 1), jnp.float32))
    carry = unit(block, carry, True)
    carry = lax.fori_loop(0, block, lambda i, c: unit(block - 1 - i, c, False), carry)
    out_ref[0] = carry[0].astype(out_ref.dtype)


def attention(data, place, share, span):
    blocks, _, size = data.shape
    width = min(256, span)
    index = jnp.arange(width)
    tri = (index[:, None] > index[None, :]).astype(jnp.bfloat16)
    work = blocks * (blocks + 1) // 2 * share * span
    return pl.pallas_call(
        functools.partial(attention_kernel, share, span),
        grid=(blocks,),
        in_specs=[
            pl.BlockSpec(memory_space=pltpu.SMEM),
            pl.BlockSpec(memory_space=pltpu.VMEM),
            pl.BlockSpec(memory_space=pltpu.VMEM),
        ],
        out_specs=pl.BlockSpec((1, share, size), lambda i: (i, 0, 0)),
        out_shape=jax.ShapeDtypeStruct((blocks, share, size), jnp.bfloat16),
        cost_estimate=pl.CostEstimate(
            flops=work * (4 * size + 2 * width),
            bytes_accessed=data.size * 2,
            transcendentals=3 * work,
        ),
        compiler_params=pltpu.CompilerParams(
            dimension_semantics=("arbitrary",), vmem_limit_bytes=40 * 1024 * 1024
        ),
        name="stick",
    )(place, data, tri)


def body(
    queries,
    keys,
    values,
    key_bias,
    out_weight,
    moe_input,
    moe_gain,
    route_ids,
    route_scores,
    shared_gate,
    shared_up,
    shared_down,
    expert_gate,
    expert_up,
    expert_down,
):
    span = queries.shape[0]
    heads = key_bias.shape[1]
    size = queries.shape[1] // heads
    ep_count = lax.axis_size("ep")
    tp_count = lax.axis_size("tp")
    groups = ep_count // heads
    share = span // groups
    place = (lax.axis_index("ep") % groups).astype(jnp.int32).reshape(1)

    def spread(array):
        return jnp.broadcast_to(array[:, None], (heads, groups) + array.shape[1:]).reshape(
            (ep_count,) + array.shape[1:]
        )

    query_parts = (
        queries.reshape(groups, share, heads, size)
        .transpose(2, 0, 1, 3)
        .reshape(ep_count, share, size)
    )
    key_parts = spread(keys.reshape(span, heads, size).transpose(1, 0, 2))
    value_parts = spread(values.reshape(span, heads, size).transpose(1, 0, 2))
    bias_parts = key_bias.T.reshape(heads, span // size, size)
    bias_parts = spread(jnp.pad(bias_parts, ((0, 0), (0, BIAS_ROWS - span // size), (0, 0))))
    data = lax.all_to_all(
        jnp.concatenate([query_parts, key_parts, value_parts, bias_parts], axis=1),
        "ep",
        split_axis=0,
        concat_axis=0,
        tiled=True,
    )
    mixed_heads = attention(data, place, share, span)
    mixed_heads = lax.all_to_all(mixed_heads, "ep", split_axis=0, concat_axis=0, tiled=True)
    heads_out = (
        mixed_heads.reshape(heads, groups, share, size)
        .transpose(1, 2, 0, 3)
        .reshape(span, heads * size)
    )
    col_count = out_weight.shape[1] // tp_count
    weight_cols = lax.all_to_all(
        out_weight.reshape(-1, tp_count, col_count).transpose(1, 0, 2),
        "tp",
        split_axis=0,
        concat_axis=0,
        tiled=True,
    )
    heads_all = lax.all_gather(heads_out, "tp", axis=0)
    mixed_tokens = jnp.einsum(
        "trh,thd->rd", heads_all, weight_cols, preferred_element_type=jnp.float32
    ).astype(jnp.bfloat16)

    token_count = moe_input.shape[0]
    inputs = moe_input.astype(jnp.float32)
    normed = (
        inputs * lax.rsqrt(jnp.mean(inputs * inputs, axis=-1, keepdims=True) + EPS_NORM) * moe_gain
    ).astype(jnp.bfloat16)
    own_cols = lax.dynamic_slice_in_dim(normed, lax.axis_index("tp") * col_count, col_count, 1)
    shared_hidden = (
        jax.nn.silu(jnp.dot(normed, shared_gate, preferred_element_type=jnp.float32))
        * jnp.dot(normed, shared_up, preferred_element_type=jnp.float32)
    ).astype(jnp.bfloat16)
    local_experts = expert_gate.shape[0]
    expert_count = local_experts * ep_count
    topk = route_ids.shape[1]
    capacity = 3 * token_count * topk // (2 * expert_count)
    send_slots = expert_count * capacity
    onehot = route_ids[:, :, None] == jnp.arange(expert_count, dtype=jnp.int32)
    named = jnp.sum(onehot.astype(jnp.bfloat16), axis=1)
    row = jnp.arange(token_count)
    earlier = jnp.dot(
        (row[:, None] > row[None, :]).astype(jnp.bfloat16),
        named,
        preferred_element_type=jnp.float32,
    ).astype(jnp.int32)
    place_in = jnp.sum(jnp.where(onehot, earlier[:, None, :], 0), axis=2)
    slot_ids = route_ids * capacity + place_in
    matches = slot_ids[None] == jnp.arange(send_slots, dtype=jnp.int32)[:, None, None]
    dispatch = jnp.sum(matches.astype(jnp.bfloat16), axis=2)
    outgoing = jnp.dot(dispatch, own_cols, preferred_element_type=jnp.float32).astype(jnp.bfloat16)
    arrived = lax.all_to_all(outgoing, "ep", split_axis=0, concat_axis=0, tiled=True)
    piece = lax.all_gather(arrived, "tp", axis=1, tiled=True)
    width = piece.shape[1]
    grid = piece.reshape(ep_count, local_experts, capacity, width)
    gate_sum = jnp.einsum("secd,edf->secf", grid, expert_gate, preferred_element_type=jnp.float32)
    up_sum = jnp.einsum("secd,edf->secf", grid, expert_up, preferred_element_type=jnp.float32)
    expert_hidden = (jax.nn.silu(gate_sum) * up_sum).astype(jnp.bfloat16)
    routed = jnp.einsum(
        "secf,efd->dsec", expert_hidden, expert_down, preferred_element_type=jnp.float32
    ).reshape(tp_count * col_count, -1)
    common = jnp.einsum("tf,fd->dt", shared_hidden, shared_down, preferred_element_type=jnp.float32)
    expert_sum = lax.psum_scatter(
        jnp.concatenate([routed, common], axis=1).astype(jnp.bfloat16),
        "tp",
        scatter_dimension=0,
        tiled=True,
    )
    routed_sum = expert_sum[:, :send_slots]
    common_sum = expert_sum[:, send_slots:].astype(jnp.float32)
    returned = lax.all_to_all(routed_sum, "ep", split_axis=1, concat_axis=1, tiled=True)
    gates = route_scores / jnp.sum(route_scores, axis=-1, keepdims=True) * ROUTED_SCALE
    gates_high = gates.astype(jnp.bfloat16)
    gates_low = (gates - gates_high.astype(jnp.float32)).astype(jnp.bfloat16)

    def combined(part):
        table = jnp.sum(jnp.where(matches, part[None], jnp.bfloat16(0)), axis=2)
        return jnp.einsum("ds,st->td", returned, table, preferred_element_type=jnp.float32)

    expert_mix = (common_sum.T + combined(gates_high) + combined(gates_low)).astype(jnp.bfloat16)
    return (mixed_tokens, expert_mix)


def solution(mesh):
    return jax.shard_map(
        body,
        mesh=mesh,
        in_specs=(
            P("ep", "tp"),
            P("ep", "tp"),
            P("ep", "tp"),
            P("ep", "tp"),
            P("tp", None),
            P("ep", None),
            P(),
            P("ep", None),
            P("ep", None),
            P(None, "tp"),
            P(None, "tp"),
            P("tp", None),
            P("ep", None, "tp"),
            P("ep", None, "tp"),
            P("ep", "tp", None),
        ),
        out_specs=(P("ep", "tp"), P("ep", "tp")),
        check_vma=False,
    )
```

```python
import functools

import jax
import jax.numpy as jnp
from jax import lax
from jax.experimental import pallas as pl
from jax.experimental.pallas import tpu as pltpu
from jax.sharding import PartitionSpec as P

EPS_NORM = 1e-06
ROUTED_SCALE = 2.5
LOG2E = 1.4426950408889634
BIAS_ROWS = 16
MESH = pl.DeviceIdType.MESH


def attention_kernel(place_ref, query_ref, key_ref, value_ref, bias_ref, tri_ref, out_ref):
    block = pl.program_id(0)
    share, size = query_ref.shape[1:]
    span = key_ref.shape[1]
    offset = place_ref[0] * share
    width = tri_ref.shape[0]
    query = query_ref[block]
    scale = size ** (-0.5) * LOG2E

    def unit(key_block, carry, masked):
        total, passed = carry
        key = key_ref[key_block]
        value = value_ref[key_block]
        bias = bias_ref[key_block].astype(jnp.float32) * LOG2E
        for start in range(span - width, -1, -width):
            row = jnp.concatenate(
                [bias[i : i + 1, :] for i in range(start // size, (start + width) // size)],
                axis=1,
            )
            logit = (
                lax.dot_general(
                    query,
                    key[start : start + width],
                    (((1,), (1,)), ((), ())),
                    preferred_element_type=jnp.float32,
                )
                * scale
                + row
            )
            drop = jnp.maximum(logit, jnp.log(1.0 + jnp.exp2(jnp.minimum(logit, 126.0))) * LOG2E)
            base = logit - drop
            if masked:
                shape = (share, width)
                visible = start + lax.broadcasted_iota(
                    jnp.int32, shape, 1
                ) < offset + lax.broadcasted_iota(jnp.int32, shape, 0)
                drop = jnp.where(visible, drop, 0.0)
            later = jnp.dot(
                drop.astype(jnp.bfloat16), tri_ref[...], preferred_element_type=jnp.float32
            )
            weight = jnp.exp2(base - later - passed)
            if masked:
                weight = jnp.where(visible, weight, 0.0)
            passed = passed + later[:, 0:1] + drop[:, 0:1]
            total = total + jnp.dot(
                weight.astype(jnp.bfloat16),
                value[start : start + width],
                preferred_element_type=jnp.float32,
            )
        return (total, passed)

    carry = (jnp.zeros((share, size), jnp.float32), jnp.zeros((share, 1), jnp.float32))
    carry = unit(block, carry, True)
    carry = lax.fori_loop(0, block, lambda i, c: unit(block - 1 - i, c, False), carry)
    out_ref[0] = carry[0].astype(out_ref.dtype)


def attention(query, key, value, bias, place):
    blocks, share, size = query.shape
    span = key.shape[1]
    width = min(256, span)
    index = jnp.arange(width)
    tri = (index[:, None] > index[None, :]).astype(jnp.bfloat16)
    work = blocks * (blocks + 1) // 2 * share * span
    whole = pl.BlockSpec(memory_space=pltpu.VMEM)
    return pl.pallas_call(
        attention_kernel,
        grid=(blocks,),
        in_specs=[pl.BlockSpec(memory_space=pltpu.SMEM)] + [whole] * 5,
        out_specs=pl.BlockSpec((1, share, size), lambda i: (i, 0, 0)),
        out_shape=jax.ShapeDtypeStruct((blocks, share, size), jnp.bfloat16),
        cost_estimate=pl.CostEstimate(
            flops=work * (4 * size + 2 * width),
            bytes_accessed=key.size * 5,
            transcendentals=3 * work,
        ),
        compiler_params=pltpu.CompilerParams(
            dimension_semantics=("arbitrary",), vmem_limit_bytes=40 * 1024 * 1024
        ),
        name="stick",
    )(place, query, key, value, bias, tri)


def columns(index, width):
    return pl.ds(pl.multiple_of(index * width, width), width)


def meet(ep_count, tp_count):
    own_ep, own_tp = lax.axis_index("ep"), lax.axis_index("tp")
    barrier = pltpu.get_barrier_semaphore()
    for i in range(1, ep_count):
        pl.semaphore_signal(
            barrier, inc=1, device_id={"ep": lax.rem(own_ep + i, ep_count)}, device_id_type=MESH
        )
    for i in range(1, tp_count):
        pl.semaphore_signal(
            barrier, inc=1, device_id={"tp": lax.rem(own_tp + i, tp_count)}, device_id_type=MESH
        )
    pl.semaphore_wait(barrier, ep_count + tp_count - 2)


def exchange_kernel(
    counts,
    query_ref,
    key_ref,
    value_ref,
    bias_ref,
    rows_ref,
    weight_ref,
    query_out,
    key_out,
    value_out,
    bias_out,
    rows_out,
    weight_out,
    local_sem,
    query_send,
    query_recv,
    part_send,
    part_recv,
    rows_send,
    rows_recv,
    relay_send,
    relay_recv,
    weight_send,
    weight_recv,
):
    ep_count, tp_count, heads = counts
    groups = ep_count // heads
    share, size = query_out.shape[1:]
    depth = weight_ref.shape[0]
    col_count = weight_out.shape[1]
    own, own_tp = lax.axis_index("ep"), lax.axis_index("tp")
    own_head, own_group = own // groups, lax.rem(own, groups)
    rows_own = rows_out.at[:, :, columns(own_tp, col_count)]

    def query_part(device):
        return query_ref.at[columns(lax.rem(device, groups), share), columns(device // groups, size)]

    def part(kind, head):
        if kind == 2:
            return bias_ref.at[head]
        return (key_ref, value_ref)[kind].at[:, columns(head, size)]

    part_outs = (key_out, value_out, bias_out)

    def remote(source, target, send, recv, axis, device):
        return pltpu.make_async_remote_copy(
            src_ref=source,
            dst_ref=target,
            send_sem=send,
            recv_sem=recv,
            device_id={axis: device},
            device_id_type=MESH,
        )

    meet(ep_count, tp_count)
    sent = []

    def start(copy):
        copy.start()
        sent.append(copy)

    local = [
        pltpu.make_async_copy(rows_ref.at[own], rows_out.at[own, :, columns(own_tp, col_count)], local_sem.at[0]),
        pltpu.make_async_copy(query_part(own), query_out.at[own], local_sem.at[1]),
        pltpu.make_async_copy(
            weight_ref.at[:, columns(own_tp, col_count)],
            weight_out.at[columns(own_tp, depth), :],
            local_sem.at[2],
        ),
    ] + [
        pltpu.make_async_copy(part(kind, own_head), part_outs[kind].at[own], local_sem.at[3 + kind])
        for kind in range(3)
    ]
    for copy in local:
        copy.start()
    for i in range(1, ep_count):
        other = lax.rem(own + i, ep_count)
        start(
            remote(
                rows_ref.at[other],
                rows_out.at[own, :, columns(own_tp, col_count)],
                rows_send.at[other],
                rows_recv.at[own],
                "ep",
                other,
            )
        )
    for step in range(1, groups):
        group = lax.rem(own_group + step, groups)
        other = own_head * groups + group
        for kind in range(3):
            start(
                remote(
                    part(kind, own_head),
                    part_outs[kind].at[own],
                    part_send.at[kind, other],
                    part_recv.at[kind, own],
                    "ep",
                    other,
                )
            )
    for i in range(1, heads):
        head = lax.rem(own_head + i, heads)
        other = head * groups + own_group
        for kind in range(3):
            start(
                remote(
                    part(kind, head),
                    part_outs[kind].at[own],
                    part_send.at[kind, other],
                    part_recv.at[kind, own],
                    "ep",
                    other,
                )
            )
    for i in range(1, ep_count):
        other = lax.rem(own + i, ep_count)
        start(
            remote(
                query_part(other),
                query_out.at[own],
                query_send.at[other],
                query_recv.at[own],
                "ep",
                other,
            )
        )
    for i in range(1, ep_count):
        other = lax.rem(own + i, ep_count)
        remote(
            rows_ref.at[other],
            rows_out.at[other, :, columns(own_tp, col_count)],
            rows_send.at[other],
            rows_recv.at[other],
            "ep",
            other,
        ).wait_recv()
    local[0].wait()
    for i in range(1, tp_count):
        other = lax.rem(own_tp + i, tp_count)
        start(remote(rows_own, rows_own, relay_send.at[other], relay_recv.at[own_tp], "tp", other))
    for i in range(1, tp_count):
        other = lax.rem(own_tp + i, tp_count)
        start(
            remote(
                weight_ref.at[:, columns(other, col_count)],
                weight_out.at[columns(own_tp, depth), :],
                weight_send.at[other],
                weight_recv.at[own_tp],
                "tp",
                other,
            )
        )

    def part_arrival(kind, source):
        target = part_outs[kind].at[source]
        remote(
            target, target, part_send.at[kind, source], part_recv.at[kind, source], "ep", source
        ).wait_recv()

    for i in range(1, heads):
        source = lax.rem(own_head + heads - i, heads) * groups + own_group
        for kind in range(3):
            part_arrival(kind, source)
            for step in range(1, groups):
                group = lax.rem(own_group + step, groups)
                target = part_outs[kind].at[source]
                start(
                    remote(
                        target,
                        target,
                        part_send.at[kind, source - own_group + group],
                        part_recv.at[kind, source],
                        "ep",
                        own_head * groups + group,
                    )
                )
    for i in range(heads):
        for step in range(1, groups):
            group = lax.rem(own_group + step, groups)
            source = lax.rem(own_head + heads - i, heads) * groups + group
            for kind in range(3):
                part_arrival(kind, source)
    for i in range(1, ep_count):
        other = lax.rem(own + i, ep_count)
        remote(
            query_part(other),
            query_out.at[other],
            query_send.at[other],
            query_recv.at[other],
            "ep",
            other,
        ).wait_recv()
    for i in range(1, tp_count):
        other = lax.rem(own_tp + i, tp_count)
        arrived = rows_out.at[:, :, columns(other, col_count)]
        remote(
            arrived, arrived, relay_send.at[other], relay_recv.at[other], "tp", other
        ).wait_recv()
        target = weight_out.at[columns(other, depth), :]
        remote(
            target, target, weight_send.at[other], weight_recv.at[other], "tp", other
        ).wait_recv()
    for copy in sent:
        copy.wait_send()
    for copy in local[1:]:
        copy.wait()


def exchange(queries, keys, values, bias, rows, weight, counts):
    ep_count, tp_count, heads = counts
    span = queries.shape[0]
    size = queries.shape[1] // heads
    share = span * heads // ep_count
    depth, features = weight.shape
    whole = pl.BlockSpec(memory_space=pltpu.VMEM)
    free = pl.BlockSpec(memory_space=pl.ANY)
    dma = pltpu.SemaphoreType.DMA
    kind = jnp.bfloat16
    return pl.pallas_call(
        functools.partial(exchange_kernel, counts),
        in_specs=[whole] * 6,
        out_specs=[free] * 6,
        out_shape=[
            jax.ShapeDtypeStruct((ep_count, share, size), kind),
            jax.ShapeDtypeStruct((ep_count, span, size), kind),
            jax.ShapeDtypeStruct((ep_count, span, size), kind),
            jax.ShapeDtypeStruct((ep_count,) + bias.shape[1:], kind),
            jax.ShapeDtypeStruct((ep_count, rows.shape[1], features), kind),
            jax.ShapeDtypeStruct((depth * tp_count, features // tp_count), kind),
        ],
        scratch_shapes=[
            dma((6,)),
            dma((ep_count,)),
            dma((ep_count,)),
            dma((3, ep_count)),
            dma((3, ep_count)),
            dma((ep_count,)),
            dma((ep_count,)),
            dma((tp_count,)),
            dma((tp_count,)),
            dma((tp_count,)),
            dma((tp_count,)),
        ],
        compiler_params=pltpu.CompilerParams(
            collective_id=0, has_side_effects=True, vmem_limit_bytes=40 * 1024 * 1024
        ),
        name="exchange",
    )(queries, keys, values, bias, rows, weight)


def gather_kernel(counts, part_ref, out_ref, local_sem, send_sem, recv_sem, relay_send, relay_recv):
    ep_count, tp_count, heads = counts
    groups = ep_count // heads
    share, size = part_ref.shape[1:]
    own, own_tp = lax.axis_index("ep"), lax.axis_index("tp")

    def place_of(source, slot):
        return out_ref.at[
            columns(lax.rem(source, groups), share), columns(slot * heads + source // groups, size)
        ]

    def remote(source, target, send, recv, axis, device):
        return pltpu.make_async_remote_copy(
            src_ref=source,
            dst_ref=target,
            send_sem=send,
            recv_sem=recv,
            device_id={axis: device},
            device_id_type=MESH,
        )

    meet(ep_count, tp_count)
    local = pltpu.make_async_copy(part_ref.at[own], place_of(own, own_tp), local_sem.at[0])
    local.start()
    sent = []
    for i in range(1, ep_count):
        other = lax.rem(own + i, ep_count)
        copy = remote(
            part_ref.at[other],
            place_of(own, own_tp),
            send_sem.at[other],
            recv_sem.at[own],
            "ep",
            other,
        )
        copy.start()
        sent.append(copy)
    for i in range(ep_count):
        source = lax.rem(own + ep_count - i, ep_count)
        piece = place_of(source, own_tp)
        if i == 0:
            local.wait()
        else:
            remote(
                piece, piece, send_sem.at[source], recv_sem.at[source], "ep", source
            ).wait_recv()
        for j in range(1, tp_count):
            other = lax.rem(own_tp + j, tp_count)
            copy = remote(
                piece,
                piece,
                relay_send.at[source, other],
                relay_recv.at[source, own_tp],
                "tp",
                other,
            )
            copy.start()
            sent.append(copy)
    for i in range(ep_count):
        source = lax.rem(own + ep_count - i, ep_count)
        for j in range(1, tp_count):
            other = lax.rem(own_tp + j, tp_count)
            piece = place_of(source, other)
            remote(
                piece,
                piece,
                relay_send.at[source, other],
                relay_recv.at[source, other],
                "tp",
                other,
            ).wait_recv()
    for copy in sent:
        copy.wait_send()


def gather(parts, counts):
    ep_count, tp_count, heads = counts
    _, share, size = parts.shape
    dma = pltpu.SemaphoreType.DMA
    return pl.pallas_call(
        functools.partial(gather_kernel, counts),
        in_specs=[pl.BlockSpec(memory_space=pltpu.VMEM)],
        out_specs=pl.BlockSpec(memory_space=pl.ANY),
        out_shape=jax.ShapeDtypeStruct(
            (share * ep_count // heads, tp_count * heads * size), jnp.bfloat16
        ),
        scratch_shapes=[
            dma((1,)),
            dma((ep_count,)),
            dma((ep_count,)),
            dma((ep_count, tp_count)),
            dma((ep_count, tp_count)),
        ],
        compiler_params=pltpu.CompilerParams(collective_id=1, has_side_effects=True),
        cost_estimate=pl.CostEstimate(
            flops=0, bytes_accessed=parts.size * 100, transcendentals=0
        ),
        name="gather",
    )(parts)


def body(
    queries,
    keys,
    values,
    key_bias,
    out_weight,
    moe_input,
    moe_gain,
    route_ids,
    route_scores,
    shared_gate,
    shared_up,
    shared_down,
    expert_gate,
    expert_up,
    expert_down,
):
    span = queries.shape[0]
    heads = key_bias.shape[1]
    size = queries.shape[1] // heads
    ep_count = lax.axis_size("ep")
    tp_count = lax.axis_size("tp")
    groups = ep_count // heads
    share = span // groups
    place = (lax.axis_index("ep") % groups).astype(jnp.int32).reshape(1)

    counts = (ep_count, tp_count, heads)
    col_count = out_weight.shape[1] // tp_count
    bias_parts = key_bias.T.reshape(heads, span // size, size)
    bias_parts = jnp.pad(bias_parts, ((0, 0), (0, BIAS_ROWS - span // size), (0, 0)))

    token_count = moe_input.shape[0]
    inputs = moe_input.astype(jnp.float32)
    normed = (
        inputs * lax.rsqrt(jnp.mean(inputs * inputs, axis=-1, keepdims=True) + EPS_NORM) * moe_gain
    ).astype(jnp.bfloat16)
    own_cols = lax.dynamic_slice_in_dim(normed, lax.axis_index("tp") * col_count, col_count, 1)
    shared_hidden = (
        jax.nn.silu(jnp.dot(normed, shared_gate, preferred_element_type=jnp.float32))
        * jnp.dot(normed, shared_up, preferred_element_type=jnp.float32)
    ).astype(jnp.bfloat16)
    local_experts = expert_gate.shape[0]
    expert_count = local_experts * ep_count
    topk = route_ids.shape[1]
    capacity = 3 * token_count * topk // (2 * expert_count)
    send_slots = expert_count * capacity
    onehot = route_ids[:, :, None] == jnp.arange(expert_count, dtype=jnp.int32)
    named = jnp.sum(onehot.astype(jnp.bfloat16), axis=1)
    row = jnp.arange(token_count)
    earlier = jnp.dot(
        (row[:, None] > row[None, :]).astype(jnp.bfloat16),
        named,
        preferred_element_type=jnp.float32,
    ).astype(jnp.int32)
    place_in = jnp.sum(jnp.where(onehot, earlier[:, None, :], 0), axis=2)
    slot_ids = route_ids * capacity + place_in
    matches = slot_ids[None] == jnp.arange(send_slots, dtype=jnp.int32)[:, None, None]
    dispatch = jnp.sum(matches.astype(jnp.bfloat16), axis=2)
    outgoing = jnp.dot(dispatch, own_cols, preferred_element_type=jnp.float32).astype(jnp.bfloat16)
    query_all, key_all, value_all, bias_all, grid, weight_cols = exchange(
        queries,
        keys,
        values,
        bias_parts,
        outgoing.reshape(ep_count, local_experts * capacity, col_count),
        out_weight,
        counts,
    )
    grid = grid.reshape(ep_count, local_experts, capacity, -1)
    gate_sum = jnp.einsum("secd,edf->secf", grid, expert_gate, preferred_element_type=jnp.float32)
    up_sum = jnp.einsum("secd,edf->secf", grid, expert_up, preferred_element_type=jnp.float32)
    expert_hidden = (jax.nn.silu(gate_sum) * up_sum).astype(jnp.bfloat16)
    routed = jnp.einsum(
        "secf,efd->dsec", expert_hidden, expert_down, preferred_element_type=jnp.float32
    ).reshape(tp_count * col_count, -1)
    common = jnp.einsum("tf,fd->dt", shared_hidden, shared_down, preferred_element_type=jnp.float32)
    partial = jnp.concatenate([routed, common], axis=1).astype(jnp.bfloat16)
    partial, query_all = lax.optimization_barrier((partial, query_all))
    mixed_heads = attention(query_all, key_all, value_all, bias_all, place)
    heads_all = gather(mixed_heads, counts)
    mixed_tokens = jnp.dot(heads_all, weight_cols, preferred_element_type=jnp.float32).astype(
        jnp.bfloat16
    )
    expert_sum = lax.psum_scatter(
        partial,
        "tp",
        scatter_dimension=0,
        tiled=True,
    )
    routed_sum = expert_sum[:, :send_slots]
    common_sum = expert_sum[:, send_slots:].astype(jnp.float32)
    returned = lax.all_to_all(routed_sum, "ep", split_axis=1, concat_axis=1, tiled=True)
    gates = route_scores / jnp.sum(route_scores, axis=-1, keepdims=True) * ROUTED_SCALE
    gates_high = gates.astype(jnp.bfloat16)
    gates_low = (gates - gates_high.astype(jnp.float32)).astype(jnp.bfloat16)

    def combined(part):
        table = jnp.sum(jnp.where(matches, part[None], jnp.bfloat16(0)), axis=2)
        return jnp.einsum("ds,st->td", returned, table, preferred_element_type=jnp.float32)

    expert_mix = (common_sum.T + combined(gates_high) + combined(gates_low)).astype(jnp.bfloat16)
    return (mixed_tokens, expert_mix)


def solution(mesh):
    return jax.shard_map(
        body,
        mesh=mesh,
        in_specs=(
            P("ep", "tp"),
            P("ep", "tp"),
            P("ep", "tp"),
            P("ep", "tp"),
            P("tp", None),
            P("ep", None),
            P(),
            P("ep", None),
            P("ep", None),
            P(None, "tp"),
            P(None, "tp"),
            P("tp", None),
            P("ep", None, "tp"),
            P("ep", None, "tp"),
            P("ep", "tp", None),
        ),
        out_specs=(P("ep", "tp"), P("ep", "tp")),
        check_vma=False,
    )
```

```python
import functools

import jax
import jax.numpy as jnp
from jax import lax
from jax.experimental import pallas as pl
from jax.experimental.pallas import tpu as pltpu
from jax.sharding import PartitionSpec as P

EPS_NORM = 1e-06
ROUTED_SCALE = 2.5
LOG2E = 1.4426950408889634
BIAS_ROWS = 16
MESH = pl.DeviceIdType.MESH


def attention_kernel(
    tp_count,
    query_ref,
    key_ref,
    value_ref,
    bias_ref,
    tri_ref,
    partial_ref,
    out_ref,
    partial_out,
    local_sem,
    send_sem,
    recv_sem,
):
    block = pl.program_id(0)
    own_tp = lax.axis_index("tp")
    width_out = partial_out.shape[2]
    local = pltpu.make_async_copy(
        partial_ref.at[:, columns(own_tp, width_out)], partial_out.at[own_tp], local_sem.at[0]
    )

    def piece(i, arriving):
        other = lax.rem(own_tp + i, tp_count)
        return pltpu.make_async_remote_copy(
            src_ref=partial_ref.at[:, columns(other, width_out)],
            dst_ref=partial_out.at[other if arriving else own_tp],
            send_sem=send_sem.at[other],
            recv_sem=recv_sem.at[other if arriving else own_tp],
            device_id={"tp": other},
            device_id_type=MESH,
        )

    @pl.when(block == 0)
    def _():
        barrier = pltpu.get_barrier_semaphore()
        for i in range(1, tp_count):
            pl.semaphore_signal(
                barrier,
                inc=1,
                device_id={"tp": lax.rem(own_tp + i, tp_count)},
                device_id_type=MESH,
            )
        pl.semaphore_wait(barrier, tp_count - 1)
        for i in range(1, tp_count):
            piece(i, False).start()
        local.start()

    share, size = query_ref.shape[1:]
    span = key_ref.shape[1]
    groups = span // share
    offset = lax.rem(lax.axis_index("ep"), groups) * share
    width = tri_ref.shape[0]
    query = query_ref[block]
    scale = size ** (-0.5) * LOG2E

    def unit(key_block, carry, masked):
        total, passed = carry
        key = key_ref[key_block]
        value = value_ref[key_block]
        bias = bias_ref[key_block].astype(jnp.float32) * LOG2E
        for start in range(span - width, -1, -width):
            row = jnp.concatenate(
                [bias[i : i + 1, :] for i in range(start // size, (start + width) // size)],
                axis=1,
            )
            logit = (
                lax.dot_general(
                    query,
                    key[start : start + width],
                    (((1,), (1,)), ((), ())),
                    preferred_element_type=jnp.float32,
                )
                * scale
                + row
            )
            drop = jnp.maximum(logit, jnp.log(1.0 + jnp.exp2(jnp.minimum(logit, 126.0))) * LOG2E)
            base = logit - drop
            if masked:
                shape = (share, width)
                visible = start + lax.broadcasted_iota(
                    jnp.int32, shape, 1
                ) < offset + lax.broadcasted_iota(jnp.int32, shape, 0)
                drop = jnp.where(visible, drop, 0.0)
            later = jnp.dot(
                drop.astype(jnp.bfloat16), tri_ref[...], preferred_element_type=jnp.float32
            )
            weight = jnp.exp2(base - later - passed)
            if masked:
                weight = jnp.where(visible, weight, 0.0)
            passed = passed + later[:, 0:1] + drop[:, 0:1]
            total = total + jnp.dot(
                weight.astype(jnp.bfloat16),
                value[start : start + width],
                preferred_element_type=jnp.float32,
            )
        return (total, passed)

    carry = (jnp.zeros((share, size), jnp.float32), jnp.zeros((share, 1), jnp.float32))
    carry = unit(block, carry, True)
    carry = lax.fori_loop(0, block, lambda i, c: unit(block - 1 - i, c, False), carry)
    out_ref[0] = carry[0].astype(out_ref.dtype)

    @pl.when(block == pl.num_programs(0) - 1)
    def _():
        local.wait()
        for i in range(1, tp_count):
            piece(i, True).wait_recv()
        for i in range(1, tp_count):
            piece(i, False).wait_send()


def attention(query, key, value, bias, partial, tp_count):
    blocks, share, size = query.shape
    span = key.shape[1]
    width = min(256, span)
    index = jnp.arange(width)
    tri = (index[:, None] > index[None, :]).astype(jnp.bfloat16)
    dma = pltpu.SemaphoreType.DMA
    work = blocks * (blocks + 1) // 2 * share * span
    whole = pl.BlockSpec(memory_space=pltpu.VMEM)
    return pl.pallas_call(
        functools.partial(attention_kernel, tp_count),
        grid=(blocks,),
        in_specs=[whole] * 6,
        out_specs=[
            pl.BlockSpec((1, share, size), lambda i: (i, 0, 0)),
            pl.BlockSpec(memory_space=pl.ANY),
        ],
        out_shape=[
            jax.ShapeDtypeStruct((blocks, share, size), jnp.bfloat16),
            jax.ShapeDtypeStruct(
                (tp_count, partial.shape[0], partial.shape[1] // tp_count), jnp.bfloat16
            ),
        ],
        scratch_shapes=[dma((1,)), dma((tp_count,)), dma((tp_count,))],
        cost_estimate=pl.CostEstimate(
            flops=work * (4 * size + 2 * width),
            bytes_accessed=key.size * 5,
            transcendentals=3 * work,
        ),
        compiler_params=pltpu.CompilerParams(
            dimension_semantics=("arbitrary",),
            vmem_limit_bytes=40 * 1024 * 1024,
            collective_id=2,
            has_side_effects=True,
        ),
        name="stick",
    )(query, key, value, bias, tri, partial)


def others_across(own_tp, tp_count):
    pair = 2 - tp_count % 2
    chips = tp_count // pair
    return [
        lax.rem(own_tp // pair + i, chips) * pair + lax.rem(own_tp, pair) for i in range(1, chips)
    ]


def beside(own_tp, tp_count):
    if tp_count % 2:
        return []
    return [own_tp + 1 - 2 * lax.rem(own_tp, 2)]


def near_first(own_tp, tp_count):
    return others_across(own_tp, tp_count) + beside(own_tp, tp_count)


def columns(index, width):
    return pl.ds(pl.multiple_of(index * width, width), width)


def meet(ep_count, tp_count):
    own_ep, own_tp = lax.axis_index("ep"), lax.axis_index("tp")
    barrier = pltpu.get_barrier_semaphore()
    for i in range(1, ep_count):
        pl.semaphore_signal(
            barrier, inc=1, device_id={"ep": lax.rem(own_ep + i, ep_count)}, device_id_type=MESH
        )
    for i in range(1, tp_count):
        pl.semaphore_signal(
            barrier, inc=1, device_id={"tp": lax.rem(own_tp + i, tp_count)}, device_id_type=MESH
        )
    pl.semaphore_wait(barrier, ep_count + tp_count - 2)


def exchange_kernel(
    counts,
    query_ref,
    key_ref,
    value_ref,
    bias_ref,
    rows_ref,
    weight_ref,
    query_out,
    key_out,
    value_out,
    bias_out,
    rows_out,
    weight_out,
    local_sem,
    query_send,
    query_recv,
    part_send,
    part_recv,
    rows_send,
    rows_recv,
    relay_send,
    relay_recv,
    pass_send,
    weight_send,
    weight_recv,
):
    ep_count, tp_count, heads = counts
    groups = ep_count // heads
    share, size = query_out.shape[1:]
    depth = weight_ref.shape[0]
    col_count = weight_out.shape[1]
    own, own_tp = lax.axis_index("ep"), lax.axis_index("tp")
    own_head, own_group = own // groups, lax.rem(own, groups)
    rows_own = rows_out.at[:, :, columns(own_tp, col_count)]

    def query_part(device):
        return query_ref.at[columns(lax.rem(device, groups), share), columns(device // groups, size)]

    def part(kind, head):
        if kind == 2:
            return bias_ref.at[head]
        return (key_ref, value_ref)[kind].at[:, columns(head, size)]

    part_outs = (key_out, value_out, bias_out)

    def remote(source, target, send, recv, axis, device):
        return pltpu.make_async_remote_copy(
            src_ref=source,
            dst_ref=target,
            send_sem=send,
            recv_sem=recv,
            device_id={axis: device},
            device_id_type=MESH,
        )

    meet(ep_count, tp_count)
    sent = []

    def start(copy):
        copy.start()
        sent.append(copy)

    local = [
        pltpu.make_async_copy(rows_ref.at[own], rows_out.at[own, :, columns(own_tp, col_count)], local_sem.at[0]),
        pltpu.make_async_copy(query_part(own), query_out.at[own], local_sem.at[1]),
        pltpu.make_async_copy(
            weight_ref.at[:, columns(own_tp, col_count)],
            weight_out.at[columns(own_tp, depth), :],
            local_sem.at[2],
        ),
    ] + [
        pltpu.make_async_copy(part(kind, own_head), part_outs[kind].at[own], local_sem.at[3 + kind])
        for kind in range(3)
    ]
    for copy in local:
        copy.start()
    for i in range(1, ep_count):
        other = lax.rem(own + i, ep_count)
        start(
            remote(
                rows_ref.at[other],
                rows_out.at[own, :, columns(own_tp, col_count)],
                rows_send.at[other],
                rows_recv.at[own],
                "ep",
                other,
            )
        )
    for step in range(1, groups):
        group = lax.rem(own_group + step, groups)
        other = own_head * groups + group
        for kind in range(3):
            start(
                remote(
                    part(kind, own_head),
                    part_outs[kind].at[own],
                    part_send.at[kind, other],
                    part_recv.at[kind, own],
                    "ep",
                    other,
                )
            )
    for i in range(1, heads):
        head = lax.rem(own_head + i, heads)
        other = head * groups + own_group
        for kind in range(3):
            start(
                remote(
                    part(kind, head),
                    part_outs[kind].at[own],
                    part_send.at[kind, other],
                    part_recv.at[kind, own],
                    "ep",
                    other,
                )
            )
    for i in range(1, ep_count):
        other = lax.rem(own + i, ep_count)
        start(
            remote(
                query_part(other),
                query_out.at[own],
                query_send.at[other],
                query_recv.at[own],
                "ep",
                other,
            )
        )
    for i in range(1, ep_count):
        other = lax.rem(own + i, ep_count)
        remote(
            rows_ref.at[other],
            rows_out.at[other, :, columns(own_tp, col_count)],
            rows_send.at[other],
            rows_recv.at[other],
            "ep",
            other,
        ).wait_recv()
    local[0].wait()
    for other in near_first(own_tp, tp_count):
        start(remote(rows_own, rows_own, relay_send.at[other], relay_recv.at[own_tp], "tp", other))
    for i in range(1, tp_count):
        other = lax.rem(own_tp + i, tp_count)
        start(
            remote(
                weight_ref.at[:, columns(other, col_count)],
                weight_out.at[columns(own_tp, depth), :],
                weight_send.at[other],
                weight_recv.at[own_tp],
                "tp",
                other,
            )
        )

    def part_arrival(kind, source):
        target = part_outs[kind].at[source]
        remote(
            target, target, part_send.at[kind, source], part_recv.at[kind, source], "ep", source
        ).wait_recv()

    for i in range(1, heads):
        source = lax.rem(own_head + heads - i, heads) * groups + own_group
        for kind in range(3):
            part_arrival(kind, source)
            for step in range(1, groups):
                group = lax.rem(own_group + step, groups)
                target = part_outs[kind].at[source]
                start(
                    remote(
                        target,
                        target,
                        part_send.at[kind, source - own_group + group],
                        part_recv.at[kind, source],
                        "ep",
                        own_head * groups + group,
                    )
                )
    def rows_arrival(slot):
        arrived = rows_out.at[:, :, columns(slot, col_count)]
        remote(
            arrived, arrived, relay_send.at[slot], relay_recv.at[slot], "tp", slot
        ).wait_recv()
        return arrived

    for slot in others_across(own_tp, tp_count):
        arrived = rows_arrival(slot)
        for other in beside(own_tp, tp_count):
            start(
                remote(arrived, arrived, pass_send.at[slot], relay_recv.at[slot], "tp", other)
            )
    for i in range(heads):
        for step in range(1, groups):
            group = lax.rem(own_group + step, groups)
            source = lax.rem(own_head + heads - i, heads) * groups + group
            for kind in range(3):
                part_arrival(kind, source)
    for i in range(1, ep_count):
        other = lax.rem(own + i, ep_count)
        remote(
            query_part(other),
            query_out.at[other],
            query_send.at[other],
            query_recv.at[other],
            "ep",
            other,
        ).wait_recv()
    for i in range(1, tp_count):
        other = lax.rem(own_tp + i, tp_count)
        target = weight_out.at[columns(other, depth), :]
        remote(
            target, target, weight_send.at[other], weight_recv.at[other], "tp", other
        ).wait_recv()
    for other in beside(own_tp, tp_count):
        rows_arrival(other)
        for slot in others_across(other, tp_count):
            rows_arrival(slot)
    for copy in sent:
        copy.wait_send()
    for copy in local[1:]:
        copy.wait()


def exchange(queries, keys, values, bias, rows, weight, counts):
    ep_count, tp_count, heads = counts
    span = queries.shape[0]
    size = queries.shape[1] // heads
    share = span * heads // ep_count
    depth, features = weight.shape
    whole = pl.BlockSpec(memory_space=pltpu.VMEM)
    free = pl.BlockSpec(memory_space=pl.ANY)
    dma = pltpu.SemaphoreType.DMA
    kind = jnp.bfloat16
    return pl.pallas_call(
        functools.partial(exchange_kernel, counts),
        in_specs=[whole] * 6,
        out_specs=[free] * 6,
        out_shape=[
            jax.ShapeDtypeStruct((ep_count, share, size), kind),
            jax.ShapeDtypeStruct((ep_count, span, size), kind),
            jax.ShapeDtypeStruct((ep_count, span, size), kind),
            jax.ShapeDtypeStruct((ep_count,) + bias.shape[1:], kind),
            jax.ShapeDtypeStruct((ep_count, rows.shape[1], features), kind),
            jax.ShapeDtypeStruct((depth * tp_count, features // tp_count), kind),
        ],
        scratch_shapes=[
            dma((6,)),
            dma((ep_count,)),
            dma((ep_count,)),
            dma((3, ep_count)),
            dma((3, ep_count)),
            dma((ep_count,)),
            dma((ep_count,)),
            dma((tp_count,)),
            dma((tp_count,)),
            dma((tp_count,)),
            dma((tp_count,)),
            dma((tp_count,)),
        ],
        compiler_params=pltpu.CompilerParams(
            collective_id=0, has_side_effects=True, vmem_limit_bytes=40 * 1024 * 1024
        ),
        name="exchange",
    )(queries, keys, values, bias, rows, weight)


def gather_kernel(
    counts,
    part_ref,
    back_ref,
    out_ref,
    back_out,
    local_sem,
    send_sem,
    recv_sem,
    relay_send,
    relay_recv,
    pass_send,
    back_send,
    back_recv,
):
    ep_count, tp_count, heads = counts
    groups = ep_count // heads
    share, size = part_ref.shape[1:]
    own, own_tp = lax.axis_index("ep"), lax.axis_index("tp")

    def place_of(source, slot):
        return out_ref.at[
            columns(lax.rem(source, groups), share), columns(slot * heads + source // groups, size)
        ]

    def remote(source, target, send, recv, axis, device):
        return pltpu.make_async_remote_copy(
            src_ref=source,
            dst_ref=target,
            send_sem=send,
            recv_sem=recv,
            device_id={axis: device},
            device_id_type=MESH,
        )

    meet(ep_count, tp_count)
    local = pltpu.make_async_copy(part_ref.at[own], place_of(own, own_tp), local_sem.at[0])
    local.start()
    local_back = pltpu.make_async_copy(back_ref.at[own], back_out.at[own], local_sem.at[1])
    local_back.start()
    sent = []

    def start(copy):
        copy.start()
        sent.append(copy)

    for i in range(1, ep_count):
        other = lax.rem(own + i, ep_count)
        start(
            remote(
                part_ref.at[other],
                place_of(own, own_tp),
                send_sem.at[other],
                recv_sem.at[own],
                "ep",
                other,
            )
        )
    for i in range(1, ep_count):
        other = lax.rem(own + i, ep_count)
        start(
            remote(
                back_ref.at[other],
                back_out.at[own],
                back_send.at[other],
                back_recv.at[own],
                "ep",
                other,
            )
        )
    sources = [lax.rem(own + ep_count - i, ep_count) for i in range(ep_count)]
    for i, source in enumerate(sources):
        piece = place_of(source, own_tp)
        if i == 0:
            local.wait()
        else:
            remote(
                piece, piece, send_sem.at[source], recv_sem.at[source], "ep", source
            ).wait_recv()
        for other in near_first(own_tp, tp_count):
            start(
                remote(
                    piece,
                    piece,
                    relay_send.at[source, other],
                    relay_recv.at[source, own_tp],
                    "tp",
                    other,
                )
            )

    def arrival(source, slot):
        piece = place_of(source, slot)
        remote(
            piece, piece, relay_send.at[source, slot], relay_recv.at[source, slot], "tp", slot
        ).wait_recv()
        return piece

    for source in sources:
        for slot in others_across(own_tp, tp_count):
            piece = arrival(source, slot)
            for other in beside(own_tp, tp_count):
                start(
                    remote(
                        piece,
                        piece,
                        pass_send.at[source, slot],
                        relay_recv.at[source, slot],
                        "tp",
                        other,
                    )
                )
    for source in sources:
        for other in beside(own_tp, tp_count):
            arrival(source, other)
            for slot in others_across(other, tp_count):
                arrival(source, slot)
    for source in sources[1:]:
        remote(
            back_ref.at[source],
            back_out.at[source],
            back_send.at[source],
            back_recv.at[source],
            "ep",
            source,
        ).wait_recv()
    for copy in sent:
        copy.wait_send()
    local_back.wait()


def gather(parts, back, counts):
    ep_count, tp_count, heads = counts
    _, share, size = parts.shape
    dma = pltpu.SemaphoreType.DMA
    return pl.pallas_call(
        functools.partial(gather_kernel, counts),
        in_specs=[pl.BlockSpec(memory_space=pltpu.VMEM)] * 2,
        out_specs=[pl.BlockSpec(memory_space=pl.ANY)] * 2,
        out_shape=[
            jax.ShapeDtypeStruct(
                (share * ep_count // heads, tp_count * heads * size), jnp.bfloat16
            ),
            jax.ShapeDtypeStruct(back.shape, jnp.bfloat16),
        ],
        scratch_shapes=[
            dma((2,)),
            dma((ep_count,)),
            dma((ep_count,)),
            dma((ep_count, tp_count)),
            dma((ep_count, tp_count)),
            dma((ep_count, tp_count)),
            dma((ep_count,)),
            dma((ep_count,)),
        ],
        compiler_params=pltpu.CompilerParams(collective_id=1, has_side_effects=True),
        cost_estimate=pl.CostEstimate(
            flops=0, bytes_accessed=parts.size * 100, transcendentals=0
        ),
        name="gather",
    )(parts, back)


def body(
    queries,
    keys,
    values,
    key_bias,
    out_weight,
    moe_input,
    moe_gain,
    route_ids,
    route_scores,
    shared_gate,
    shared_up,
    shared_down,
    expert_gate,
    expert_up,
    expert_down,
):
    span = queries.shape[0]
    heads = key_bias.shape[1]
    size = queries.shape[1] // heads
    ep_count = lax.axis_size("ep")
    tp_count = lax.axis_size("tp")

    counts = (ep_count, tp_count, heads)
    col_count = out_weight.shape[1] // tp_count
    bias_parts = key_bias.T.reshape(heads, span // size, size)
    bias_parts = jnp.pad(bias_parts, ((0, 0), (0, BIAS_ROWS - span // size), (0, 0)))

    token_count = moe_input.shape[0]
    inputs = moe_input.astype(jnp.float32)
    normed = (
        inputs * lax.rsqrt(jnp.mean(inputs * inputs, axis=-1, keepdims=True) + EPS_NORM) * moe_gain
    ).astype(jnp.bfloat16)
    own_cols = lax.dynamic_slice_in_dim(normed, lax.axis_index("tp") * col_count, col_count, 1)
    shared_hidden = (
        jax.nn.silu(jnp.dot(normed, shared_gate, preferred_element_type=jnp.float32))
        * jnp.dot(normed, shared_up, preferred_element_type=jnp.float32)
    ).astype(jnp.bfloat16)
    local_experts = expert_gate.shape[0]
    expert_count = local_experts * ep_count
    topk = route_ids.shape[1]
    capacity = 3 * token_count * topk // (2 * expert_count)
    send_slots = expert_count * capacity
    onehot = route_ids[:, :, None] == jnp.arange(expert_count, dtype=jnp.int32)
    named = jnp.sum(onehot.astype(jnp.bfloat16), axis=1)
    row = jnp.arange(token_count)
    earlier = jnp.dot(
        (row[:, None] > row[None, :]).astype(jnp.bfloat16),
        named,
        preferred_element_type=jnp.float32,
    ).astype(jnp.int32)
    place_in = jnp.sum(jnp.where(onehot, earlier[:, None, :], 0), axis=2)
    slot_ids = route_ids * capacity + place_in
    matches = slot_ids[None] == jnp.arange(send_slots, dtype=jnp.int32)[:, None, None]
    dispatch = jnp.sum(matches.astype(jnp.bfloat16), axis=2)
    outgoing = jnp.dot(dispatch, own_cols, preferred_element_type=jnp.float32).astype(jnp.bfloat16)
    query_all, key_all, value_all, bias_all, grid, weight_cols = exchange(
        queries,
        keys,
        values,
        bias_parts,
        outgoing.reshape(ep_count, local_experts * capacity, col_count),
        out_weight,
        counts,
    )
    grid = grid.reshape(ep_count, local_experts, capacity, -1)
    gate_sum = jnp.einsum("secd,edf->secf", grid, expert_gate, preferred_element_type=jnp.float32)
    up_sum = jnp.einsum("secd,edf->secf", grid, expert_up, preferred_element_type=jnp.float32)
    expert_hidden = (jax.nn.silu(gate_sum) * up_sum).astype(jnp.bfloat16)
    routed = jnp.einsum(
        "secf,efd->secd", expert_hidden, expert_down, preferred_element_type=jnp.float32
    ).reshape(send_slots, -1)
    common = jnp.dot(shared_hidden, shared_down, preferred_element_type=jnp.float32)
    partial = jnp.concatenate([routed, common], axis=0).astype(jnp.bfloat16)
    mixed_heads, partial_all = attention(
        query_all, key_all, value_all, bias_all, partial, tp_count
    )
    expert_sum = jnp.sum(partial_all.astype(jnp.float32), axis=0)
    routed_sum = expert_sum[:send_slots].astype(jnp.bfloat16)
    common_sum = expert_sum[send_slots:]
    heads_all, returned = gather(
        mixed_heads, routed_sum.reshape(ep_count, local_experts * capacity, col_count), counts
    )
    returned = returned.reshape(send_slots, col_count)
    mixed_tokens = jnp.dot(heads_all, weight_cols, preferred_element_type=jnp.float32).astype(
        jnp.bfloat16
    )
    gates = route_scores / jnp.sum(route_scores, axis=-1, keepdims=True) * ROUTED_SCALE
    gates_high = gates.astype(jnp.bfloat16)
    gates_low = (gates - gates_high.astype(jnp.float32)).astype(jnp.bfloat16)

    def combined(part):
        table = jnp.sum(jnp.where(matches, part[None], jnp.bfloat16(0)), axis=2)
        return jnp.einsum("st,sd->td", table, returned, preferred_element_type=jnp.float32)

    expert_mix = (common_sum + combined(gates_high) + combined(gates_low)).astype(jnp.bfloat16)
    return (mixed_tokens, expert_mix)


def solution(mesh):
    return jax.shard_map(
        body,
        mesh=mesh,
        in_specs=(
            P("ep", "tp"),
            P("ep", "tp"),
            P("ep", "tp"),
            P("ep", "tp"),
            P("tp", None),
            P("ep", None),
            P(),
            P("ep", None),
            P("ep", None),
            P(None, "tp"),
            P(None, "tp"),
            P("tp", None),
            P("ep", None, "tp"),
            P("ep", None, "tp"),
            P("ep", "tp", None),
        ),
        out_specs=(P("ep", "tp"), P("ep", "tp")),
        check_vma=False,
    )
```

```python
import functools

import jax
import jax.numpy as jnp
from jax import lax
from jax.experimental import pallas as pl
from jax.experimental.pallas import tpu as pltpu
from jax.sharding import PartitionSpec as P

EPS_NORM = 1e-06
ROUTED_SCALE = 2.5
LOG2E = 1.4426950408889634
BIAS_ROWS = 16
MESH = pl.DeviceIdType.MESH


def attention_kernel(
    tp_count,
    query_ref,
    key_ref,
    value_ref,
    bias_ref,
    tri_ref,
    partial_ref,
    out_ref,
    partial_out,
    out_buf,
    local_sem,
    send_sem,
    recv_sem,
    out_send,
    out_recv,
):
    block = pl.program_id(0)
    ep_count = key_ref.shape[0]
    own = lax.axis_index("ep")
    own_tp = lax.axis_index("tp")
    width_out = partial_out.shape[2]
    local = pltpu.make_async_copy(
        partial_ref.at[:, columns(own_tp, width_out)], partial_out.at[own_tp], local_sem.at[0]
    )

    def piece(i, arriving):
        other = lax.rem(own_tp + i, tp_count)
        return pltpu.make_async_remote_copy(
            src_ref=partial_ref.at[:, columns(other, width_out)],
            dst_ref=partial_out.at[other if arriving else own_tp],
            send_sem=send_sem.at[other],
            recv_sem=recv_sem.at[other if arriving else own_tp],
            device_id={"tp": other},
            device_id_type=MESH,
        )

    @pl.when(block == 0)
    def _():
        meet(ep_count, tp_count)
        for i in range(1, tp_count):
            piece(i, False).start()
        local.start()

    share, size = query_ref.shape[1:]
    span = key_ref.shape[1]
    groups = span // share
    offset = lax.rem(lax.axis_index("ep"), groups) * share
    width = tri_ref.shape[0]
    query = query_ref[block]
    scale = size ** (-0.5) * LOG2E

    def unit(key_block, carry, masked):
        total, passed = carry
        key = key_ref[key_block]
        value = value_ref[key_block]
        bias = bias_ref[key_block].astype(jnp.float32) * LOG2E
        for start in range(span - width, -1, -width):
            row = jnp.concatenate(
                [bias[i : i + 1, :] for i in range(start // size, (start + width) // size)],
                axis=1,
            )
            logit = (
                lax.dot_general(
                    query,
                    key[start : start + width],
                    (((1,), (1,)), ((), ())),
                    preferred_element_type=jnp.float32,
                )
                * scale
                + row
            )
            drop = jnp.maximum(logit, jnp.log(1.0 + jnp.exp2(jnp.minimum(logit, 126.0))) * LOG2E)
            base = logit - drop
            if masked:
                shape = (share, width)
                visible = start + lax.broadcasted_iota(
                    jnp.int32, shape, 1
                ) < offset + lax.broadcasted_iota(jnp.int32, shape, 0)
                drop = jnp.where(visible, drop, 0.0)
            later = jnp.dot(
                drop.astype(jnp.bfloat16), tri_ref[...], preferred_element_type=jnp.float32
            )
            weight = jnp.exp2(base - later - passed)
            if masked:
                weight = jnp.where(visible, weight, 0.0)
            passed = passed + later[:, 0:1] + drop[:, 0:1]
            total = total + jnp.dot(
                weight.astype(jnp.bfloat16),
                value[start : start + width],
                preferred_element_type=jnp.float32,
            )
        return (total, passed)

    carry = (jnp.zeros((share, size), jnp.float32), jnp.zeros((share, 1), jnp.float32))
    carry = unit(block, carry, True)
    carry = lax.fori_loop(0, block, lambda i, c: unit(block - 1 - i, c, False), carry)
    out_buf[block] = carry[0].astype(out_buf.dtype)

    def place_of(source):
        return out_ref.at[columns(lax.rem(source, groups), share), columns(source // groups, size)]

    def result(owner, source):
        return pltpu.make_async_remote_copy(
            src_ref=out_buf.at[owner],
            dst_ref=place_of(source),
            send_sem=out_send.at[owner],
            recv_sem=out_recv.at[source],
            device_id={"ep": owner},
            device_id_type=MESH,
        )

    local_out = pltpu.make_async_copy(out_buf.at[own], place_of(own), local_sem.at[1])

    def leave(owner):
        @pl.when(owner == own)
        def _():
            local_out.start()

        @pl.when(owner != own)
        def _():
            result(owner, own).start()

    @pl.when(block > 0)
    def _():
        leave(block - 1)

    @pl.when(block == pl.num_programs(0) - 1)
    def _():
        local.wait()
        leave(block)
        for i in range(1, ep_count):
            other = lax.rem(own + i, ep_count)
            result(other, other).wait_recv()
        for i in range(1, ep_count):
            result(lax.rem(own + i, ep_count), own).wait_send()
        local_out.wait()
        for i in range(1, tp_count):
            piece(i, True).wait_recv()
        for i in range(1, tp_count):
            piece(i, False).wait_send()


def attention(query, key, value, bias, partial, tp_count):
    blocks, share, size = query.shape
    span = key.shape[1]
    width = min(256, span)
    index = jnp.arange(width)
    tri = (index[:, None] > index[None, :]).astype(jnp.bfloat16)
    dma = pltpu.SemaphoreType.DMA
    work = blocks * (blocks + 1) // 2 * share * span
    whole = pl.BlockSpec(memory_space=pltpu.VMEM)
    return pl.pallas_call(
        functools.partial(attention_kernel, tp_count),
        grid=(blocks,),
        in_specs=[whole] * 6,
        out_specs=[
            pl.BlockSpec(memory_space=pl.ANY),
            pl.BlockSpec(memory_space=pl.ANY),
        ],
        out_shape=[
            jax.ShapeDtypeStruct((span, blocks * share // span * size), jnp.bfloat16),
            jax.ShapeDtypeStruct(
                (tp_count, partial.shape[0], partial.shape[1] // tp_count), jnp.bfloat16
            ),
        ],
        scratch_shapes=[
            pltpu.VMEM((blocks, share, size), jnp.bfloat16),
            dma((2,)),
            dma((tp_count,)),
            dma((tp_count,)),
            dma((blocks,)),
            dma((blocks,)),
        ],
        cost_estimate=pl.CostEstimate(
            flops=work * (4 * size + 2 * width),
            bytes_accessed=key.size * 5,
            transcendentals=3 * work,
        ),
        compiler_params=pltpu.CompilerParams(
            dimension_semantics=("arbitrary",),
            vmem_limit_bytes=40 * 1024 * 1024,
            collective_id=2,
            has_side_effects=True,
        ),
        name="stick",
    )(query, key, value, bias, tri, partial)


def others_across(own_tp, tp_count):
    pair = 2 - tp_count % 2
    chips = tp_count // pair
    return [
        lax.rem(own_tp // pair + i, chips) * pair + lax.rem(own_tp, pair) for i in range(1, chips)
    ]


def beside(own_tp, tp_count):
    if tp_count % 2:
        return []
    return [own_tp + 1 - 2 * lax.rem(own_tp, 2)]


def near_first(own_tp, tp_count):
    return others_across(own_tp, tp_count) + beside(own_tp, tp_count)


def columns(index, width):
    return pl.ds(pl.multiple_of(index * width, width), width)


def meet(ep_count, tp_count):
    own_ep, own_tp = lax.axis_index("ep"), lax.axis_index("tp")
    barrier = pltpu.get_barrier_semaphore()
    for i in range(1, ep_count):
        pl.semaphore_signal(
            barrier, inc=1, device_id={"ep": lax.rem(own_ep + i, ep_count)}, device_id_type=MESH
        )
    for i in range(1, tp_count):
        pl.semaphore_signal(
            barrier, inc=1, device_id={"tp": lax.rem(own_tp + i, tp_count)}, device_id_type=MESH
        )
    pl.semaphore_wait(barrier, ep_count + tp_count - 2)


def exchange_kernel(
    counts,
    query_ref,
    key_ref,
    value_ref,
    bias_ref,
    rows_ref,
    weight_ref,
    query_out,
    key_out,
    value_out,
    bias_out,
    rows_out,
    weight_out,
    local_sem,
    query_send,
    query_recv,
    part_send,
    part_recv,
    rows_send,
    rows_recv,
    relay_send,
    relay_recv,
    pass_send,
    weight_send,
    weight_recv,
):
    ep_count, tp_count, heads = counts
    groups = ep_count // heads
    share, size = query_out.shape[1:]
    depth = weight_ref.shape[0]
    col_count = weight_out.shape[1]
    own, own_tp = lax.axis_index("ep"), lax.axis_index("tp")
    own_head, own_group = own // groups, lax.rem(own, groups)
    rows_own = rows_out.at[:, :, columns(own_tp, col_count)]

    def query_part(device):
        return query_ref.at[columns(lax.rem(device, groups), share), columns(device // groups, size)]

    def part(kind, head):
        if kind == 2:
            return bias_ref.at[head]
        return (key_ref, value_ref)[kind].at[:, columns(head, size)]

    part_outs = (key_out, value_out, bias_out)

    def remote(source, target, send, recv, axis, device):
        return pltpu.make_async_remote_copy(
            src_ref=source,
            dst_ref=target,
            send_sem=send,
            recv_sem=recv,
            device_id={axis: device},
            device_id_type=MESH,
        )

    meet(ep_count, tp_count)
    sent = []

    def start(copy):
        copy.start()
        sent.append(copy)

    local = [
        pltpu.make_async_copy(rows_ref.at[own], rows_out.at[own, :, columns(own_tp, col_count)], local_sem.at[0]),
        pltpu.make_async_copy(query_part(own), query_out.at[own], local_sem.at[1]),
        pltpu.make_async_copy(
            weight_ref.at[:, columns(own_tp, col_count)],
            weight_out.at[columns(own_tp, depth), :],
            local_sem.at[2],
        ),
    ] + [
        pltpu.make_async_copy(part(kind, own_head), part_outs[kind].at[own], local_sem.at[3 + kind])
        for kind in range(3)
    ]
    for copy in local:
        copy.start()
    for i in range(1, ep_count):
        other = lax.rem(own + i, ep_count)
        start(
            remote(
                rows_ref.at[other],
                rows_out.at[own, :, columns(own_tp, col_count)],
                rows_send.at[other],
                rows_recv.at[own],
                "ep",
                other,
            )
        )
    for step in range(1, groups):
        group = lax.rem(own_group + step, groups)
        other = own_head * groups + group
        for kind in range(3):
            start(
                remote(
                    part(kind, own_head),
                    part_outs[kind].at[own],
                    part_send.at[kind, other],
                    part_recv.at[kind, own],
                    "ep",
                    other,
                )
            )
    for i in range(1, heads):
        head = lax.rem(own_head + i, heads)
        other = head * groups + own_group
        for kind in range(3):
            start(
                remote(
                    part(kind, head),
                    part_outs[kind].at[own],
                    part_send.at[kind, other],
                    part_recv.at[kind, own],
                    "ep",
                    other,
                )
            )
    for i in range(1, ep_count):
        other = lax.rem(own + i, ep_count)
        start(
            remote(
                query_part(other),
                query_out.at[own],
                query_send.at[other],
                query_recv.at[own],
                "ep",
                other,
            )
        )
    for i in range(1, ep_count):
        other = lax.rem(own + i, ep_count)
        remote(
            rows_ref.at[other],
            rows_out.at[other, :, columns(own_tp, col_count)],
            rows_send.at[other],
            rows_recv.at[other],
            "ep",
            other,
        ).wait_recv()
    local[0].wait()
    for other in near_first(own_tp, tp_count):
        start(remote(rows_own, rows_own, relay_send.at[other], relay_recv.at[own_tp], "tp", other))
    for i in range(1, tp_count):
        other = lax.rem(own_tp + i, tp_count)
        start(
            remote(
                weight_ref.at[:, columns(other, col_count)],
                weight_out.at[columns(own_tp, depth), :],
                weight_send.at[other],
                weight_recv.at[own_tp],
                "tp",
                other,
            )
        )

    def part_arrival(kind, source):
        target = part_outs[kind].at[source]
        remote(
            target, target, part_send.at[kind, source], part_recv.at[kind, source], "ep", source
        ).wait_recv()

    for i in range(1, heads):
        source = lax.rem(own_head + heads - i, heads) * groups + own_group
        for kind in range(3):
            part_arrival(kind, source)
            for step in range(1, groups):
                group = lax.rem(own_group + step, groups)
                target = part_outs[kind].at[source]
                start(
                    remote(
                        target,
                        target,
                        part_send.at[kind, source - own_group + group],
                        part_recv.at[kind, source],
                        "ep",
                        own_head * groups + group,
                    )
                )
    def rows_arrival(slot):
        arrived = rows_out.at[:, :, columns(slot, col_count)]
        remote(
            arrived, arrived, relay_send.at[slot], relay_recv.at[slot], "tp", slot
        ).wait_recv()
        return arrived

    for slot in others_across(own_tp, tp_count):
        arrived = rows_arrival(slot)
        for other in beside(own_tp, tp_count):
            start(
                remote(arrived, arrived, pass_send.at[slot], relay_recv.at[slot], "tp", other)
            )
    for i in range(heads):
        for step in range(1, groups):
            group = lax.rem(own_group + step, groups)
            source = lax.rem(own_head + heads - i, heads) * groups + group
            for kind in range(3):
                part_arrival(kind, source)
    for i in range(1, ep_count):
        other = lax.rem(own + i, ep_count)
        remote(
            query_part(other),
            query_out.at[other],
            query_send.at[other],
            query_recv.at[other],
            "ep",
            other,
        ).wait_recv()
    for i in range(1, tp_count):
        other = lax.rem(own_tp + i, tp_count)
        target = weight_out.at[columns(other, depth), :]
        remote(
            target, target, weight_send.at[other], weight_recv.at[other], "tp", other
        ).wait_recv()
    for other in beside(own_tp, tp_count):
        rows_arrival(other)
        for slot in others_across(other, tp_count):
            rows_arrival(slot)
    for copy in sent:
        copy.wait_send()
    for copy in local[1:]:
        copy.wait()


def exchange(queries, keys, values, bias, rows, weight, counts):
    ep_count, tp_count, heads = counts
    span = queries.shape[0]
    size = queries.shape[1] // heads
    share = span * heads // ep_count
    depth, features = weight.shape
    whole = pl.BlockSpec(memory_space=pltpu.VMEM)
    free = pl.BlockSpec(memory_space=pl.ANY)
    dma = pltpu.SemaphoreType.DMA
    kind = jnp.bfloat16
    return pl.pallas_call(
        functools.partial(exchange_kernel, counts),
        in_specs=[whole] * 6,
        out_specs=[free] * 6,
        out_shape=[
            jax.ShapeDtypeStruct((ep_count, share, size), kind),
            jax.ShapeDtypeStruct((ep_count, span, size), kind),
            jax.ShapeDtypeStruct((ep_count, span, size), kind),
            jax.ShapeDtypeStruct((ep_count,) + bias.shape[1:], kind),
            jax.ShapeDtypeStruct((ep_count, rows.shape[1], features), kind),
            jax.ShapeDtypeStruct((depth * tp_count, features // tp_count), kind),
        ],
        scratch_shapes=[
            dma((6,)),
            dma((ep_count,)),
            dma((ep_count,)),
            dma((3, ep_count)),
            dma((3, ep_count)),
            dma((ep_count,)),
            dma((ep_count,)),
            dma((tp_count,)),
            dma((tp_count,)),
            dma((tp_count,)),
            dma((tp_count,)),
            dma((tp_count,)),
        ],
        compiler_params=pltpu.CompilerParams(
            collective_id=0, has_side_effects=True, vmem_limit_bytes=40 * 1024 * 1024
        ),
        name="exchange",
    )(queries, keys, values, bias, rows, weight)


def gather_kernel(
    counts,
    part_ref,
    back_ref,
    out_ref,
    back_out,
    local_sem,
    relay_send,
    relay_recv,
    pass_send,
    back_send,
    back_recv,
):
    ep_count, tp_count, heads = counts
    groups = ep_count // heads
    depth = part_ref.shape[1]
    own, own_tp = lax.axis_index("ep"), lax.axis_index("tp")

    def place_of(slot):
        return out_ref.at[:, columns(slot, depth)]

    def remote(source, target, send, recv, axis, device):
        return pltpu.make_async_remote_copy(
            src_ref=source,
            dst_ref=target,
            send_sem=send,
            recv_sem=recv,
            device_id={axis: device},
            device_id_type=MESH,
        )

    meet(ep_count, tp_count)
    local = pltpu.make_async_copy(part_ref, place_of(own_tp), local_sem.at[0])
    local.start()
    local_back = pltpu.make_async_copy(back_ref.at[own], back_out.at[own], local_sem.at[1])
    local_back.start()
    sent = []

    def start(copy):
        copy.start()
        sent.append(copy)

    for other in near_first(own_tp, tp_count):
        start(
            remote(
                part_ref,
                place_of(own_tp),
                relay_send.at[other],
                relay_recv.at[own_tp],
                "tp",
                other,
            )
        )
    for i in range(1, ep_count):
        other = lax.rem(own + i, ep_count)
        start(
            remote(
                back_ref.at[other],
                back_out.at[own],
                back_send.at[other],
                back_recv.at[own],
                "ep",
                other,
            )
        )
    def arrival(slot):
        piece = place_of(slot)
        remote(
            piece, piece, relay_send.at[slot], relay_recv.at[slot], "tp", slot
        ).wait_recv()
        return piece

    for slot in others_across(own_tp, tp_count):
        piece = arrival(slot)
        for other in beside(own_tp, tp_count):
            start(remote(piece, piece, pass_send.at[slot], relay_recv.at[slot], "tp", other))
    for other in beside(own_tp, tp_count):
        arrival(other)
        for slot in others_across(other, tp_count):
            arrival(slot)
    for i in range(1, ep_count):
        source = lax.rem(own + i, ep_count)
        remote(
            back_ref.at[source],
            back_out.at[source],
            back_send.at[source],
            back_recv.at[source],
            "ep",
            source,
        ).wait_recv()
    for copy in sent:
        copy.wait_send()
    local.wait()
    local_back.wait()


def gather(parts, back, counts):
    ep_count, tp_count, heads = counts
    dma = pltpu.SemaphoreType.DMA
    return pl.pallas_call(
        functools.partial(gather_kernel, counts),
        in_specs=[pl.BlockSpec(memory_space=pltpu.VMEM)] * 2,
        out_specs=[pl.BlockSpec(memory_space=pl.ANY)] * 2,
        out_shape=[
            jax.ShapeDtypeStruct(
                (parts.shape[0], tp_count * parts.shape[1]), jnp.bfloat16
            ),
            jax.ShapeDtypeStruct(back.shape, jnp.bfloat16),
        ],
        scratch_shapes=[
            dma((2,)),
            dma((tp_count,)),
            dma((tp_count,)),
            dma((tp_count,)),
            dma((ep_count,)),
            dma((ep_count,)),
        ],
        compiler_params=pltpu.CompilerParams(collective_id=1, has_side_effects=True),
        cost_estimate=pl.CostEstimate(
            flops=0, bytes_accessed=parts.size * 100, transcendentals=0
        ),
        name="gather",
    )(parts, back)


def body(
    queries,
    keys,
    values,
    key_bias,
    out_weight,
    moe_input,
    moe_gain,
    route_ids,
    route_scores,
    shared_gate,
    shared_up,
    shared_down,
    expert_gate,
    expert_up,
    expert_down,
):
    span = queries.shape[0]
    heads = key_bias.shape[1]
    size = queries.shape[1] // heads
    ep_count = lax.axis_size("ep")
    tp_count = lax.axis_size("tp")

    counts = (ep_count, tp_count, heads)
    col_count = out_weight.shape[1] // tp_count
    bias_parts = key_bias.T.reshape(heads, span // size, size)
    bias_parts = jnp.pad(bias_parts, ((0, 0), (0, BIAS_ROWS - span // size), (0, 0)))

    token_count = moe_input.shape[0]
    inputs = moe_input.astype(jnp.float32)
    normed = (
        inputs * lax.rsqrt(jnp.mean(inputs * inputs, axis=-1, keepdims=True) + EPS_NORM) * moe_gain
    ).astype(jnp.bfloat16)
    own_cols = lax.dynamic_slice_in_dim(normed, lax.axis_index("tp") * col_count, col_count, 1)
    shared_hidden = (
        jax.nn.silu(jnp.dot(normed, shared_gate, preferred_element_type=jnp.float32))
        * jnp.dot(normed, shared_up, preferred_element_type=jnp.float32)
    ).astype(jnp.bfloat16)
    local_experts = expert_gate.shape[0]
    expert_count = local_experts * ep_count
    topk = route_ids.shape[1]
    capacity = 3 * token_count * topk // (2 * expert_count)
    send_slots = expert_count * capacity
    onehot = route_ids[:, :, None] == jnp.arange(expert_count, dtype=jnp.int32)
    named = jnp.sum(onehot.astype(jnp.bfloat16), axis=1)
    row = jnp.arange(token_count)
    earlier = jnp.dot(
        (row[:, None] > row[None, :]).astype(jnp.bfloat16),
        named,
        preferred_element_type=jnp.float32,
    ).astype(jnp.int32)
    place_in = jnp.sum(jnp.where(onehot, earlier[:, None, :], 0), axis=2)
    slot_ids = route_ids * capacity + place_in
    matches = slot_ids[None] == jnp.arange(send_slots, dtype=jnp.int32)[:, None, None]
    dispatch = jnp.sum(matches.astype(jnp.bfloat16), axis=2)
    outgoing = jnp.dot(dispatch, own_cols, preferred_element_type=jnp.float32).astype(jnp.bfloat16)
    query_all, key_all, value_all, bias_all, grid, weight_cols = exchange(
        queries,
        keys,
        values,
        bias_parts,
        outgoing.reshape(ep_count, local_experts * capacity, col_count),
        out_weight,
        counts,
    )
    grid = grid.reshape(ep_count, local_experts, capacity, -1)
    gate_sum = jnp.einsum("secd,edf->secf", grid, expert_gate, preferred_element_type=jnp.float32)
    up_sum = jnp.einsum("secd,edf->secf", grid, expert_up, preferred_element_type=jnp.float32)
    expert_hidden = (jax.nn.silu(gate_sum) * up_sum).astype(jnp.bfloat16)
    routed = jnp.einsum(
        "secf,efd->secd", expert_hidden, expert_down, preferred_element_type=jnp.float32
    ).reshape(send_slots, -1)
    common = jnp.dot(shared_hidden, shared_down, preferred_element_type=jnp.float32)
    partial = jnp.concatenate([routed, common], axis=0).astype(jnp.bfloat16)
    mixed_heads, partial_all = attention(
        query_all, key_all, value_all, bias_all, partial, tp_count
    )
    expert_sum = jnp.sum(partial_all.astype(jnp.float32), axis=0)
    routed_sum = expert_sum[:send_slots].astype(jnp.bfloat16)
    common_sum = expert_sum[send_slots:]
    heads_all, returned = gather(
        mixed_heads, routed_sum.reshape(ep_count, local_experts * capacity, col_count), counts
    )
    returned = returned.reshape(send_slots, col_count)
    mixed_tokens = jnp.dot(heads_all, weight_cols, preferred_element_type=jnp.float32).astype(
        jnp.bfloat16
    )
    gates = route_scores / jnp.sum(route_scores, axis=-1, keepdims=True) * ROUTED_SCALE
    gates_high = gates.astype(jnp.bfloat16)
    gates_low = (gates - gates_high.astype(jnp.float32)).astype(jnp.bfloat16)

    def combined(part):
        table = jnp.sum(jnp.where(matches, part[None], jnp.bfloat16(0)), axis=2)
        return jnp.einsum("st,sd->td", table, returned, preferred_element_type=jnp.float32)

    expert_mix = (common_sum + combined(gates_high) + combined(gates_low)).astype(jnp.bfloat16)
    return (mixed_tokens, expert_mix)


def solution(mesh):
    return jax.shard_map(
        body,
        mesh=mesh,
        in_specs=(
            P("ep", "tp"),
            P("ep", "tp"),
            P("ep", "tp"),
            P("ep", "tp"),
            P("tp", None),
            P("ep", None),
            P(),
            P("ep", None),
            P("ep", None),
            P(None, "tp"),
            P(None, "tp"),
            P("tp", None),
            P("ep", None, "tp"),
            P("ep", None, "tp"),
            P("ep", "tp", None),
        ),
        out_specs=(P("ep", "tp"), P("ep", "tp")),
        check_vma=False,
    )
```
